32 devices in a mesh: ep: 32 (over z, y, x, core).
Axes of the slice: x: 2, y: 2, z: 4, core: 2. Of those that a mesh axis runs over, the one named last changes fastest.
Arguments:
- tokens: bfloat16 [32, 2048], P('ep'), may hold values from -6 to 6
- mixer_gain: float32 [2048], replicated, may hold values from 0.1 to 1.9
- query_weight: bfloat16 [2048, 2048], P(None, 'ep'), may hold values from -0.125 to 0.125
- key_weight: bfloat16 [2048, 2048], P(None, 'ep'), may hold values from -0.125 to 0.125
- value_weight: bfloat16 [2048, 2048], P(None, 'ep'), may hold values from -0.125 to 0.125
- outgate_weight: bfloat16 [2048, 2048], P(None, 'ep'), may hold values from -0.125 to 0.125
- input_weight: bfloat16 [2048, 4], replicated, may hold values from -0.125 to 0.125
- forget_weight: bfloat16 [2048, 4], replicated, may hold values from -0.125 to 0.125
- forget_bias: float32 [4], replicated, may hold values from 0 to 4
- memory_matrix: float32 [32, 4, 512, 512], P('ep'), may hold values from -0.3 to 0.3
- memory_norm: float32 [32, 4, 512], P('ep'), may hold values from -0.3 to 0.3
- memory_max: float32 [32, 4], P('ep'), may hold values from -2 to 2
- mixer_out: bfloat16 [2048, 2048], P(None, 'ep'), may hold values from -0.125 to 0.125
- expert_gain: float32 [2048], replicated, may hold values from 0.1 to 1.9
- expert_gate: bfloat16 [32, 2048, 1024], P('ep'), may hold values from -0.125 to 0.125
- expert_up: bfloat16 [32, 2048, 1024], P('ep'), may hold values from -0.125 to 0.125
- expert_down: bfloat16 [32, 1024, 2048], P('ep'), may hold values from -0.1875 to 0.1875
- route_group: int32 [32], P('ep'), may hold values from 0 to 3
- route_member: int32 [32, 2], P('ep'), may hold values from 0 to 7, as said below
- group_weight: float32 [32], P('ep'), may hold values from 0.25 to 1
- member_weight: float32 [32, 2], P('ep'), may hold values from 0.1 to 1
Outputs:
- layer_out: bfloat16 [32, 2048], P('ep')
- next_matrix: float32 [32, 4, 512, 512], P('ep')
- next_norm: float32 [32, 4, 512], P('ep')
- next_max: float32 [32, 4], P('ep')
The draws below stay inside these ranges and needn't reach their ends.
Inputs may be any that keep to these rules, and one draw needn't show every extreme that they name: A row's 2 experts, numbered route_group * 8 + route_member, are different members of the one group that route_group names. No expert is named by more than 4 rows in all, and one expert is named by exactly 4 rows.
All inputs are finite; a program needn't handle non-finite values.
Results may differ from the reference program's by a relative error of at most 0.013.
Values may be sent and summed in bfloat16 or wider, within the bound.
A program may use at most 64 MiB of HBM per device.

```python
import math
import jax
import jax.numpy as jnp
from jax import lax

D = 2048
HEADS = 4
HEAD_DIM = 512
FF = 1024
GROUPS = 4
TOP_K = 2
SEQ_DEV = 1
TOKENS = 32
EXPERTS = 32
MEMBERS = 8
CAPACITY = 4


def route_tables(key):
    base = jax.random.fold_in(key, 11)
    streams = jax.random.split(base, 4)
    favour = jax.random.randint(streams[0], (EXPERTS,), 0, 64)
    hottest = jax.random.randint(streams[1], (), 0, EXPERTS)
    noise = jax.random.randint(streams[2], (TOKENS, EXPERTS), 0, 64)
    column = jnp.arange(EXPERTS, dtype=jnp.int32)
    row_index = jnp.arange(TOKENS, dtype=jnp.int32)
    score = noise + 2 * favour[None, :] + jnp.where(column == hottest, 4096, 0)[None, :]
    forced = jnp.where((row_index[:, None] == 0) & (column[None, :] == EXPERTS // 2), 16384, 0)
    forced = forced + jnp.where((row_index[:, None] == SEQ_DEV) & (column[None, :] == 0), 16384, 0)
    score = (score + forced) * EXPERTS + column[None, :]
    ranking = jax.random.permutation(streams[3], TOKENS).astype(jnp.int32)
    ranking = jnp.where(row_index == 0, -2, jnp.where(row_index == SEQ_DEV, -1, ranking))
    order = jnp.argsort(ranking).astype(jnp.int32)

    def visit(load, row):
        open_slots = load < CAPACITY
        masked = jnp.where(open_slots, score[row], -1)
        counts = jnp.sum(open_slots.reshape(GROUPS, MEMBERS).astype(jnp.int32), axis=1)
        best = jnp.where(counts >= TOP_K, jnp.max(masked.reshape(GROUPS, MEMBERS), axis=1), -1 - jnp.arange(GROUPS, dtype=jnp.int32))
        group_pick = lax.top_k(best, 1)[1][0].astype(jnp.int32)
        inside = lax.dynamic_slice_in_dim(masked, group_pick * MEMBERS, MEMBERS)
        picks = lax.top_k(inside, TOP_K)[1].astype(jnp.int32)
        load = load.at[group_pick * MEMBERS + picks].add(1)
        return (load, (group_pick, picks))
    _, (groups_seen, members_seen) = lax.scan(visit, jnp.zeros((EXPERTS,), jnp.int32), order)
    group_ids = jnp.zeros((TOKENS,), jnp.int32).at[order].set(groups_seen)
    member_ids = jnp.zeros((TOKENS, TOP_K), jnp.int32).at[order].set(members_seen)
    return (group_ids, member_ids)


def draw_route_group(key, part):
    return route_tables(key)[0]


def draw_route_member(key, part):
    return route_tables(key)[1]


def steps_of(key, shape, pieces, smallest, top_value):
    def one(position, blocks):
        steps = jax.random.uniform(jax.random.fold_in(jax.random.fold_in(key, 6), position), (blocks,), jnp.float32, smallest / len(pieces), top_value / len(pieces))
        return jnp.repeat(jnp.exp(steps), shape[position] // blocks).reshape((-1,) + (1,) * (len(shape) - position - 1))

    loudness = one(*pieces[0])
    for cut in pieces[1:]:
        loudness = loudness * one(*cut)
    return loudness


def scatter_about(rng, extent, width, reach, cuts=(), kind=jnp.bfloat16):
    level = steps_of(rng, extent, cuts, -0.22, 0.18) if cuts else 1.0
    drawn = jax.random.normal(rng, extent, jnp.float32) * width * level
    return jnp.minimum(jnp.maximum(drawn, -reach), reach).astype(kind)


def setup_inputs(seed: int = 0) -> dict:
    arg_keys = jax.random.split(jax.random.key(seed), 22)
    return {
        "tokens": scatter_about(arg_keys[0], (TOKENS, D), 1.0, 6.0, ((0, 32),)),
        "mixer_gain": jnp.clip(1.0 + 0.18 * jax.random.normal(arg_keys[1], (D,), jnp.float32), 0.1, 1.9),
        "query_weight": scatter_about(arg_keys[2], (D, D), D ** -0.5, 0.125, ((1, 32),)),
        "key_weight": scatter_about(arg_keys[3], (D, D), D ** -0.5, 0.125, ((1, 32),)),
        "value_weight": scatter_about(arg_keys[4], (D, D), D ** -0.5, 0.125, ((1, 32),)),
        "outgate_weight": scatter_about(arg_keys[5], (D, D), D ** -0.5, 0.125, ((1, 32),)),
        "input_weight": scatter_about(arg_keys[6], (D, HEADS), D ** -0.5, 0.125),
        "forget_weight": scatter_about(arg_keys[7], (D, HEADS), D ** -0.5, 0.125),
        "forget_bias": jnp.clip(jax.random.uniform(arg_keys[8], (HEADS,), jnp.float32, 0.0, 4.0), 0.0, 4.0),
        "memory_matrix": scatter_about(arg_keys[9], (TOKENS, HEADS, HEAD_DIM, HEAD_DIM), 0.05, 0.3, ((0, 32),), jnp.float32),
        "memory_norm": scatter_about(arg_keys[10], (TOKENS, HEADS, HEAD_DIM), 0.05, 0.3, ((0, 32),), jnp.float32),
        "memory_max": jnp.clip(jax.random.uniform(arg_keys[11], (TOKENS, HEADS), jnp.float32, -2.0, 2.0) * steps_of(arg_keys[11], (TOKENS, HEADS), ((0, 32),), -0.4, 0.0), -2.0, 2.0),
        "mixer_out": scatter_about(arg_keys[12], (D, D), D ** -0.5, 0.125, ((1, 32),)),
        "expert_gain": jnp.clip(1.0 + 0.18 * jax.random.normal(arg_keys[13], (D,), jnp.float32), 0.1, 1.9),
        "expert_gate": scatter_about(arg_keys[14], (EXPERTS, D, FF), D ** -0.5, 0.125, ((0, 32),)),
        "expert_up": scatter_about(arg_keys[15], (EXPERTS, D, FF), D ** -0.5, 0.125, ((0, 32),)),
        "expert_down": scatter_about(arg_keys[16], (EXPERTS, FF, D), FF ** -0.5, 0.1875, ((0, 32),)),
        "route_group": draw_route_group(jax.random.fold_in(arg_keys[21], 71), 0),
        "route_member": draw_route_member(jax.random.fold_in(arg_keys[21], 71), 0),
        "group_weight": jnp.clip(jnp.exp(math.log(1.0) - 1.3862944 * jax.random.uniform(arg_keys[19], (TOKENS,), jnp.float32) ** steps_of(arg_keys[19], (TOKENS,), ((0, 32),), -0.2, 0.2)), 0.25, 1.0),
        "member_weight": jnp.clip(jnp.exp(math.log(1.0) - 2.3025851 * jax.random.uniform(arg_keys[20], (TOKENS, TOP_K), jnp.float32) ** steps_of(arg_keys[20], (TOKENS, TOP_K), ((0, 32),), -0.2, 0.2)), 0.1, 1.0),
    }


norm_eps = 1e-06

def root_norm(values, gain):
    return values * lax.rsqrt(lax.optimization_barrier(jnp.mean(values * values, axis=-1, keepdims=True)) + norm_eps) * gain

def reference(tokens, mixer_gain, query_weight, key_weight, value_weight, outgate_weight, input_weight, forget_weight, forget_bias, memory_matrix, memory_norm, memory_max, mixer_out, expert_gain, expert_gate, expert_up, expert_down, route_group, route_member, group_weight, member_weight):
    count = tokens.shape[0]
    resid = tokens.astype(jnp.float32)
    normed = root_norm(resid, mixer_gain).astype(jnp.bfloat16)
    query = jnp.dot(normed, query_weight, preferred_element_type=jnp.float32).astype(jnp.bfloat16)
    key = jnp.dot(normed, key_weight, preferred_element_type=jnp.float32).astype(jnp.bfloat16)
    value = jnp.dot(normed, value_weight, preferred_element_type=jnp.float32).astype(jnp.bfloat16)
    outgate = jnp.dot(normed, outgate_weight, preferred_element_type=jnp.float32).astype(jnp.bfloat16)
    input_pre = jnp.dot(normed, input_weight, preferred_element_type=jnp.float32)
    forget_pre = jnp.dot(normed, forget_weight, preferred_element_type=jnp.float32) + forget_bias
    log_forget = jax.nn.log_sigmoid(forget_pre)
    next_max = jnp.maximum(log_forget + memory_max, input_pre)
    keep = jnp.exp(log_forget + memory_max - next_max)
    admit = jnp.exp(input_pre - next_max)
    query_heads = query.astype(jnp.float32).reshape(count, HEADS, HEAD_DIM)
    key_heads = key.astype(jnp.float32).reshape(count, HEADS, HEAD_DIM) * HEAD_DIM ** (-0.5)
    value_heads = value.astype(jnp.float32).reshape(count, HEADS, HEAD_DIM)
    carried = jnp.einsum('shij,shj->shi', memory_matrix, query_heads, precision=lax.Precision.HIGHEST)
    score = lax.optimization_barrier(jnp.sum(key_heads * query_heads, axis=-1))
    numer = keep[..., None] * carried + (admit * score)[..., None] * value_heads
    denom = keep * lax.optimization_barrier(jnp.sum(memory_norm * query_heads, axis=-1)) + admit * score
    head_out = numer / jnp.maximum(jnp.abs(denom), jnp.exp(-next_max))[..., None]
    gated = (head_out.reshape(count, D) * jax.nn.sigmoid(outgate.astype(jnp.float32))).astype(jnp.bfloat16)
    next_matrix = keep[..., None, None] * memory_matrix + admit[..., None, None] * value_heads[..., :, None] * key_heads[..., None, :]
    next_norm = keep[..., None] * memory_norm + admit[..., None] * key_heads
    projected = jnp.dot(gated, mixer_out, preferred_element_type=jnp.float32).astype(jnp.bfloat16)
    middle = (resid + projected.astype(jnp.float32)).astype(jnp.bfloat16)
    expert_in = root_norm(middle.astype(jnp.float32), expert_gain).astype(jnp.bfloat16)
    chosen = (route_group[:, None] * MEMBERS + route_member).astype(jnp.int32)
    slot_rows = jnp.repeat(jnp.arange(count, dtype=jnp.int32), TOP_K)

    def one_slot(pair):
        row_index, expert_index = pair
        row = lax.dynamic_slice_in_dim(expert_in, row_index, 1, 0)
        gate_part = jnp.dot(row, expert_gate[expert_index], preferred_element_type=jnp.float32)
        up_part = jnp.dot(row, expert_up[expert_index], preferred_element_type=jnp.float32)
        hidden = (jax.nn.silu(gate_part) * up_part).astype(jnp.bfloat16)
        return jnp.dot(hidden, expert_down[expert_index], preferred_element_type=jnp.float32).astype(jnp.bfloat16)[0]
    results = lax.map(one_slot, (slot_rows, chosen.reshape(-1))).reshape(count, TOP_K, D)
    weight = group_weight[:, None] * member_weight
    mixture = lax.optimization_barrier(jnp.sum(weight[..., None] * results.astype(jnp.float32), axis=1))
    layer_out = (middle.astype(jnp.float32) + mixture).astype(jnp.bfloat16)
    return (layer_out, next_matrix, next_norm, next_max)
```

```python
import functools

import jax
import jax.numpy as jnp
from jax import lax
from jax.experimental import pallas as pl
from jax.experimental.pallas import tpu as pltpu
from jax.sharding import PartitionSpec as P

GROUPS = 4
LANES = 128
norm_eps = 1e-06
MESH = pl.DeviceIdType.MESH
NT = (((1,), (1,)), ((), ()))


def kernel(
    n,
    cols,
    members,
    tokens_ref,
    gain_ref,
    egain_ref,
    q_hbm,
    k_hbm,
    v_hbm,
    o_hbm,
    iw_ref,
    fw_ref,
    fb_ref,
    mem_hbm,
    norm_ref,
    max_ref,
    mo_hbm,
    gate_hbm,
    up_hbm,
    down_hbm,
    group_ref,
    member_ref,
    gw_ref,
    mw_ref,
    out_ref,
    nnorm_ref,
    nmax_ref,
    key_ref,
    av_ref,
    keep_ref,
    w_in,
    w_out,
    mem,
    mem_hi,
    mem_lo,
    w_gate,
    w_up,
    w_down,
    spread,
    row16,
    sb1,
    rb1,
    sb2,
    rb2,
    x2,
    sb3,
    rb3,
    sb4,
    rb4,
    sb5,
    rb5,
    flat,
    lhs,
    middle,
    load_sem,
    send_sem,
    recv_sem,
):
    me = lax.axis_index("ep")
    width = tokens_ref.shape[1]
    blocks = width // LANES
    heads, head_dim = norm_ref.shape
    pad4 = w_in.shape[0]
    f32 = jnp.float32
    bf16 = jnp.bfloat16

    loads = []
    for src, dst in (
        (q_hbm, w_in.at[pl.ds(0, cols)]),
        (k_hbm, w_in.at[pl.ds(cols, cols)]),
        (v_hbm, w_in.at[pl.ds(2 * cols, cols)]),
        (o_hbm, w_in.at[pl.ds(3 * cols, cols)]),
        (mem_hbm, mem),
        (mo_hbm, w_out),
        (gate_hbm, w_gate),
        (up_hbm, w_up),
        (down_hbm, w_down),
    ):
        copy = pltpu.make_async_copy(src, dst, load_sem.at[len(loads)])
        copy.start()
        loads.append(copy)

    barrier = pltpu.get_barrier_semaphore()

    def greet(i, carry):
        pl.semaphore_signal(
            barrier, inc=1, device_id=(lax.rem(me + i, n),), device_id_type=MESH
        )
        return carry

    lax.fori_loop(1, n, greet, 0)

    def send_all(phase, source, target):
        def one(i, carry):
            peer = lax.rem(me + i, n)
            pltpu.make_async_remote_copy(
                src_ref=source(peer),
                dst_ref=target.at[me],
                send_sem=send_sem.at[phase],
                recv_sem=recv_sem.at[phase],
                device_id=(peer,),
                device_id_type=MESH,
            ).start()
            return carry

        lax.fori_loop(1, n, one, 0)

    def whole(phase, target):
        view = target.at[pl.ds(0, n - 1)]
        return pltpu.make_async_remote_copy(
            src_ref=view,
            dst_ref=view,
            send_sem=send_sem.at[phase],
            recv_sem=recv_sem.at[phase],
            device_id=(lax.rem(me + 1, n),),
            device_id_type=MESH,
        )

    tok = tokens_ref[...].astype(f32)
    for s in range(blocks):
        row16[pl.ds(s, 1), :] = tok[:, s * LANES : (s + 1) * LANES]
    sb1[...] = row16[...].astype(bf16)
    rb1[pl.ds(me, 1)] = sb1[...][None]

    pl.semaphore_wait(barrier, n - 1)
    send_all(0, lambda peer: sb1, rb1)

    own = row16[...]
    scale = lax.rsqrt(
        jnp.sum(jnp.sum(own * own, axis=1, keepdims=True), axis=0, keepdims=True) / width + norm_eps
    )
    own_normed = (own * scale * gain_ref[...]).astype(bf16).astype(f32)
    pre_in = jnp.zeros((heads, LANES), f32)
    pre_forget = jnp.zeros((heads, LANES), f32)
    for s in range(blocks):
        part = own_normed[s : s + 1, :]
        span = slice(s * LANES, (s + 1) * LANES)
        pre_in += iw_ref[:, span].astype(f32) * part
        pre_forget += fw_ref[:, span].astype(f32) * part
    input_pre = jnp.sum(pre_in, axis=1, keepdims=True)
    head_index = lax.broadcasted_iota(jnp.int32, (heads, 1), 0)
    bias = jnp.zeros((heads, 1), f32)
    old_max = jnp.zeros((heads, 1), f32)
    for h in range(heads):
        bias = jnp.where(head_index == h, fb_ref[h], bias)
        old_max = jnp.where(head_index == h, max_ref[0, h], old_max)
    forget_pre = jnp.sum(pre_forget, axis=1, keepdims=True) + bias
    log_forget = -(
        jnp.maximum(-forget_pre, 0.0) + jnp.log1p(jnp.exp(-jnp.abs(forget_pre)))
    )
    next_max = jnp.maximum(log_forget + old_max, input_pre)
    keep = jnp.exp(log_forget + old_max - next_max)
    admit = jnp.exp(input_pre - next_max)
    diag = lax.broadcasted_iota(jnp.int32, (heads, heads), 0) == lax.broadcasted_iota(
        jnp.int32, (heads, heads), 1
    )
    nmax_ref[...] = jnp.sum(jnp.where(diag, next_max, 0.0), axis=0, keepdims=True)
    keep_ref[...] = jnp.broadcast_to(keep, (heads, LANES))

    r_index = lax.broadcasted_iota(jnp.int32, (pad4, head_dim), 0)
    j_index = lax.broadcasted_iota(jnp.int32, (pad4, head_dim), 1)
    if cols & (cols - 1) == 0:
        same = ((r_index ^ j_index) & (cols - 1)) == 0
    else:
        same = lax.rem(r_index, cols) == lax.rem(j_index, cols)
    spread[...] = jnp.where(same, 1.0, 0.0).astype(bf16)
    if pad4 != 4 * cols:
        w_in[pl.ds(4 * cols, pad4 - 4 * cols), :] = jnp.zeros((pad4 - 4 * cols, width), bf16)

    for copy in loads[:4]:
        copy.wait()
    whole(0, rb1).wait_recv()
    rows = rb1[...].astype(f32)
    squares = jnp.sum(jnp.sum(rows * rows, axis=2, keepdims=True), axis=1, keepdims=True) / width
    normed = rows * lax.rsqrt(squares + norm_eps) * gain_ref[...][None]
    flat[...] = normed.reshape(n * blocks, LANES)
    for s in range(blocks):
        lhs[:, s * LANES : (s + 1) * LANES] = flat[pl.ds(s, n, stride=blocks), :].astype(bf16)
    result = lax.dot_general(lhs[...], w_in[...], NT, preferred_element_type=f32)
    result = result.astype(bf16).astype(f32)
    for t in range(n):
        sb2[t] = result[t : t + 1, :]
    rb2[pl.ds(me, 1)] = sb2[pl.ds(me, 1)]
    send_all(1, lambda peer: sb2.at[peer], rb2)

    loads[4].wait()
    for h in range(heads):
        block = mem[h]
        high = block.astype(bf16)
        mem_hi[h] = high
        mem_lo[h] = (block - high.astype(f32)).astype(bf16)

    whole(1, rb2).wait_recv()
    for d in range(n):
        x2[pl.ds(d, 1), :] = rb2[d]
    got = x2[...]
    lane = lax.broadcasted_iota(jnp.int32, (n, pad4), 1)
    stacked = jnp.concatenate(
        [
            jnp.where((lane >= m * cols) & (lane < (m + 1) * cols), got, 0.0).astype(bf16)
            for m in range(4)
        ],
        axis=0,
    )
    wide = jnp.dot(stacked, spread[...], preferred_element_type=f32)
    per_head = n // heads
    wide = wide.reshape(4 * heads, per_head, head_dim)
    d_index = lax.broadcasted_iota(jnp.int32, (1, per_head, head_dim), 1)
    lane = lax.broadcasted_iota(jnp.int32, (1, per_head, head_dim), 2)
    here = (lane >= d_index * cols) & (lane < (d_index + 1) * cols)
    vectors = jnp.sum(jnp.where(here, wide, 0.0), axis=1)
    query = vectors[:heads]
    key = vectors[heads : 2 * heads] * head_dim ** (-0.5)
    value = vectors[2 * heads : 3 * heads]
    outgate = vectors[3 * heads :]
    query_bf = query.astype(bf16)
    carried = []
    for h in range(heads):
        both = lax.dot_general(
            query_bf, mem_hi[h], NT, preferred_element_type=f32
        ) + lax.dot_general(query_bf, mem_lo[h], NT, preferred_element_type=f32)
        carried.append(both[h : h + 1, :])
    carried = jnp.concatenate(carried, axis=0)
    score = jnp.sum(key * query, axis=1, keepdims=True)
    old_norm = norm_ref[...]
    numer = keep * carried + (admit * score) * value
    denom = keep * jnp.sum(old_norm * query, axis=1, keepdims=True) + admit * score
    head_out = numer / jnp.maximum(jnp.abs(denom), jnp.exp(-next_max))
    gated = head_out * jax.nn.sigmoid(outgate)
    per = head_dim // LANES
    for b in range(per):
        row16[pl.ds(b, heads, stride=per), :] = gated[:, b * LANES : (b + 1) * LANES]
    sb3[...] = row16[...].astype(bf16)
    rb3[pl.ds(me, 1)] = sb3[...][None]
    send_all(2, lambda peer: sb3, rb3)
    nnorm_ref[...] = keep * old_norm + admit * key
    key_ref[...] = key
    av_ref[...] = admit * value

    loads[5].wait()
    whole(2, rb3).wait_recv()
    flat[...] = rb3[...].astype(f32).reshape(n * blocks, LANES)
    for s in range(blocks):
        lhs[:, s * LANES : (s + 1) * LANES] = flat[pl.ds(s, n, stride=blocks), :].astype(bf16)
    proj = lax.dot_general(lhs[...], w_out[...], NT, preferred_element_type=f32)
    fold = LANES // cols
    piece = n // fold
    proj = proj.astype(bf16).astype(f32)
    sb4[...] = jnp.concatenate(
        [proj[f * piece : (f + 1) * piece, :] for f in range(fold)], axis=1
    ).astype(bf16)
    rb4[pl.ds(me, 1)] = sb4[...][None]
    send_all(3, lambda peer: sb4, rb4)
    flat[...] = rb1[...].astype(f32).reshape(n * blocks, LANES)

    whole(3, rb4).wait_recv()
    lane = lax.broadcasted_iota(jnp.int32, (piece, LANES), 1)
    squares = jnp.zeros((n, LANES), f32)
    for s in range(blocks):
        pieces = [rb4[s * fold + g].astype(f32) for g in range(fold)]
        parts = []
        for f in range(fold):
            made = pieces[0] if f == 0 else pltpu.roll(pieces[0], (-f * cols) % LANES, 1)
            for g in range(1, fold):
                moved = (
                    pieces[g] if g == f else pltpu.roll(pieces[g], ((g - f) * cols) % LANES, 1)
                )
                made = jnp.where(lane >= g * cols, moved, made)
            parts.append(made)
        projected = jnp.concatenate(parts, axis=0)
        mid = (flat[pl.ds(s, n, stride=blocks), :] + projected).astype(bf16).astype(f32)
        middle[:, s * LANES : (s + 1) * LANES] = mid
        squares += mid * mid
    inverse = lax.rsqrt(jnp.sum(squares, axis=1, keepdims=True) / width + norm_eps)
    for s in range(blocks):
        span = slice(s * LANES, (s + 1) * LANES)
        lhs[:, span] = (middle[:, span] * inverse * egain_ref[pl.ds(s, 1), :]).astype(bf16)
    for copy in loads[6:]:
        copy.wait()
    gate_part = jnp.dot(lhs[...], w_gate[...], preferred_element_type=f32)
    up_part = jnp.dot(lhs[...], w_up[...], preferred_element_type=f32)
    hidden = (gate_part / (1.0 + jnp.exp(-gate_part)) * up_part).astype(bf16)
    finished = jnp.dot(hidden, w_down[...], preferred_element_type=f32)
    for s in range(blocks):
        flat[pl.ds(s, n, stride=blocks), :] = finished[:, s * LANES : (s + 1) * LANES]
    sb5[...] = flat[...].astype(bf16).reshape(n, blocks, LANES)
    rb5[pl.ds(me, 1)] = sb5[pl.ds(me, 1)]
    send_all(4, lambda peer: sb5.at[peer], rb5)

    own_middle = middle[pl.ds(me, 1), :]
    for s in range(blocks):
        row16[pl.ds(s, 1), :] = own_middle[:, s * LANES : (s + 1) * LANES]
    whole(4, rb5).wait_recv()
    mixture = jnp.zeros((blocks, LANES), f32)
    for j in range(member_ref.shape[1]):
        chosen = group_ref[0] * members + member_ref[0, j]
        weight = gw_ref[0] * mw_ref[0, j]
        mixture += weight * rb5[chosen].astype(f32)
    row16[...] = row16[...] + mixture
    final = row16[...]
    for s in range(blocks):
        out_ref[:, s * LANES : (s + 1) * LANES] = final[s : s + 1, :].astype(bf16)
    whole(0, rb1).wait_send()
    whole(1, rb2).wait_send()
    whole(2, rb3).wait_send()
    whole(3, rb4).wait_send()
    whole(4, rb5).wait_send()


def local(
    tokens,
    mixer_gain,
    query_weight,
    key_weight,
    value_weight,
    outgate_weight,
    input_weight,
    forget_weight,
    forget_bias,
    memory_matrix,
    memory_norm,
    memory_max,
    mixer_out,
    expert_gain,
    expert_gate,
    expert_up,
    expert_down,
    route_group,
    route_member,
    group_weight,
    member_weight,
):
    n = lax.axis_size("ep")
    assert tokens.shape[0] == 1 and expert_gate.shape[0] == 1
    width = tokens.shape[1]
    cols = query_weight.shape[1]
    heads, head_dim = memory_matrix.shape[1:3]
    hidden = expert_gate.shape[2]
    blocks = width // LANES
    members = n * expert_gate.shape[0] // GROUPS
    pad4 = -(-4 * cols // LANES) * LANES
    fold = LANES // cols
    f32, bf16 = jnp.float32, jnp.bfloat16
    vmem = pl.BlockSpec(memory_space=pltpu.VMEM)
    smem = pl.BlockSpec(memory_space=pltpu.SMEM)
    anym = pl.BlockSpec(memory_space=pl.ANY)
    outs = pl.pallas_call(
        functools.partial(kernel, n, cols, members),
        out_shape=(
            jax.ShapeDtypeStruct((1, width), bf16),
            jax.ShapeDtypeStruct((heads, head_dim), f32),
            jax.ShapeDtypeStruct((1, heads), f32),
            jax.ShapeDtypeStruct((heads, head_dim), f32),
            jax.ShapeDtypeStruct((heads, head_dim), f32),
            jax.ShapeDtypeStruct((heads, LANES), f32),
        ),
        in_specs=[vmem] * 3
        + [anym] * 4
        + [vmem, vmem, smem, anym, vmem, smem, anym, anym, anym, anym]
        + [smem] * 4,
        out_specs=(vmem,) * 6,
        scratch_shapes=[
            pltpu.VMEM((pad4, width), bf16),
            pltpu.VMEM((cols, width), bf16),
            pltpu.VMEM((heads, head_dim, head_dim), f32),
            pltpu.VMEM((heads, head_dim, head_dim), bf16),
            pltpu.VMEM((heads, head_dim, head_dim), bf16),
            pltpu.VMEM((width, hidden), bf16),
            pltpu.VMEM((width, hidden), bf16),
            pltpu.VMEM((hidden, width), bf16),
            pltpu.VMEM((pad4, head_dim), bf16),
            pltpu.VMEM((blocks, LANES), f32),
            pltpu.VMEM((blocks, LANES), bf16),
            pltpu.VMEM((n, blocks, LANES), bf16),
            pltpu.VMEM((n, 1, pad4), f32),
            pltpu.VMEM((n, 1, pad4), f32),
            pltpu.VMEM((n, pad4), f32),
            pltpu.VMEM((blocks, LANES), bf16),
            pltpu.VMEM((n, blocks, LANES), bf16),
            pltpu.VMEM((n // fold, LANES), bf16),
            pltpu.VMEM((n, n // fold, LANES), bf16),
            pltpu.VMEM((n, blocks, LANES), bf16),
            pltpu.VMEM((n, blocks, LANES), bf16),
            pltpu.VMEM((n * blocks, LANES), f32),
            pltpu.VMEM((n, width), bf16),
            pltpu.VMEM((n, width), f32),
            pltpu.SemaphoreType.DMA((9,)),
            pltpu.SemaphoreType.DMA((5,)),
            pltpu.SemaphoreType.DMA((5,)),
        ],
        compiler_params=pltpu.CompilerParams(
            collective_id=0, has_side_effects=True, vmem_limit_bytes=48 * 1024 * 1024
        ),
    )(
        tokens,
        mixer_gain.reshape(blocks, LANES),
        expert_gain.reshape(blocks, LANES),
        query_weight.T,
        key_weight.T,
        value_weight.T,
        outgate_weight.T,
        input_weight.T,
        forget_weight.T,
        forget_bias,
        memory_matrix[0],
        memory_norm[0],
        memory_max,
        mixer_out.T,
        expert_gate[0],
        expert_up[0],
        expert_down[0],
        route_group,
        route_member,
        group_weight,
        member_weight,
    )
    layer_out, next_norm, next_max, key, value, keep = outs
    next_matrix = (
        keep[None, :, :1, None] * memory_matrix
        + value[None, :, :, None] * key[None, :, None, :]
    )
    return (layer_out, next_matrix, next_norm[None], next_max)


def solution(mesh):
    placed = (
        P("ep", None),
        P(),
        P(None, "ep"),
        P(None, "ep"),
        P(None, "ep"),
        P(None, "ep"),
        P(),
        P(),
        P(),
        P("ep", None, None, None),
        P("ep", None, None),
        P("ep", None),
        P(None, "ep"),
        P(),
        P("ep", None, None),
        P("ep", None, None),
        P("ep", None, None),
        P("ep"),
        P("ep", None),
        P("ep"),
        P("ep", None),
    )
    return jax.shard_map(
        local,
        mesh=mesh,
        in_specs=placed,
        out_specs=(P("ep", None), P("ep", None, None, None), P("ep", None, None), P("ep", None)),
        check_vma=False,
    )
```

```python
import functools

import jax
import jax.numpy as jnp
from jax import lax
from jax.experimental import pallas as pl
from jax.experimental.pallas import tpu as pltpu
from jax.sharding import PartitionSpec as P

GROUPS = 4
LANES = 128
norm_eps = 1e-06
MESH = pl.DeviceIdType.MESH
NT = (((1,), (1,)), ((), ()))


def kernel(
    n,
    cols,
    members,
    tokens_hbm,
    gain_hbm,
    egain_hbm,
    q_hbm,
    k_hbm,
    v_hbm,
    o_hbm,
    iw_hbm,
    fw_hbm,
    fb_hbm,
    mem_hbm,
    norm_hbm,
    max_hbm,
    mo_hbm,
    gate_hbm,
    up_hbm,
    down_hbm,
    group_ref,
    member_hbm,
    gw_ref,
    mw_hbm,
    out_ref,
    nmat_ref,
    nnorm_ref,
    nmax_ref,
    tokens_ref,
    gain_ref,
    egain_ref,
    iw_ref,
    fw_ref,
    fb_ref,
    norm_ref,
    max_ref,
    member_ref,
    mw_ref,
    w_in,
    w_out,
    mem,
    mem_hi,
    mem_lo,
    w_gate,
    w_up,
    w_down,
    spread,
    row16,
    sb1,
    rb1,
    sb2,
    rb2,
    x2,
    sb3,
    rb3,
    sb4,
    rb4,
    sb5,
    rb5,
    flat,
    lhs,
    middle,
    load_sem,
    send_sem,
    recv_sem,
):
    me = lax.axis_index("ep")
    width = tokens_ref.shape[1]
    blocks = width // LANES
    heads, head_dim = norm_ref.shape
    pad4 = w_in.shape[0]
    f32 = jnp.float32
    bf16 = jnp.bfloat16

    loads = []
    for src, dst in (
        (tokens_hbm, tokens_ref),
        (gain_hbm, gain_ref),
        (iw_hbm, iw_ref),
        (fw_hbm, fw_ref),
        (fb_hbm, fb_ref),
        (max_hbm, max_ref),
        (q_hbm, w_in.at[pl.ds(0, cols)]),
        (k_hbm, w_in.at[pl.ds(cols, cols)]),
        (v_hbm, w_in.at[pl.ds(2 * cols, cols)]),
        (o_hbm, w_in.at[pl.ds(3 * cols, cols)]),
        (norm_hbm, norm_ref),
        (egain_hbm, egain_ref),
        (member_hbm, member_ref),
        (mw_hbm, mw_ref),
        (mem_hbm, mem),
        (mo_hbm, w_out),
        (gate_hbm, w_gate),
        (up_hbm, w_up),
        (down_hbm, w_down),
    ):
        copy = pltpu.make_async_copy(src, dst, load_sem.at[len(loads)])
        copy.start()
        loads.append(copy)

    barrier = pltpu.get_barrier_semaphore()

    def greet(i, carry):
        pl.semaphore_signal(
            barrier, inc=1, device_id=(lax.rem(me + i, n),), device_id_type=MESH
        )
        return carry

    lax.fori_loop(1, n, greet, 0)

    half = me // (n // 2)

    def send_all(phase, source, target):
        def one(i, carry):
            peer = lax.rem(me + half * i + (1 - half) * (n - i), n)
            pltpu.make_async_remote_copy(
                src_ref=source(peer),
                dst_ref=target.at[me],
                send_sem=send_sem.at[phase],
                recv_sem=recv_sem.at[phase],
                device_id=(peer,),
                device_id_type=MESH,
            ).start()
            return carry

        lax.fori_loop(1, n, one, 0)

    def whole(phase, target):
        view = target.at[pl.ds(0, n - 1)]
        return pltpu.make_async_remote_copy(
            src_ref=view,
            dst_ref=view,
            send_sem=send_sem.at[phase],
            recv_sem=recv_sem.at[phase],
            device_id=(lax.rem(me + 1, n),),
            device_id_type=MESH,
        )

    loads[0].wait()
    tok = tokens_ref[...].astype(f32)
    for s in range(blocks):
        row16[pl.ds(s, 1), :] = tok[:, s * LANES : (s + 1) * LANES]
    sb1[...] = row16[...].astype(bf16)
    rb1[pl.ds(me, 1)] = sb1[...][None]

    pl.semaphore_wait(barrier, n - 1)
    send_all(0, lambda peer: sb1, rb1)

    for copy in loads[1:6]:
        copy.wait()
    own = row16[...]
    scale = lax.rsqrt(
        jnp.sum(jnp.sum(own * own, axis=1, keepdims=True), axis=0, keepdims=True) / width + norm_eps
    )
    own_normed = (own * scale * gain_ref[...]).astype(bf16).astype(f32)
    pre_in = jnp.zeros((heads, LANES), f32)
    pre_forget = jnp.zeros((heads, LANES), f32)
    for s in range(blocks):
        part = own_normed[s : s + 1, :]
        span = slice(s * LANES, (s + 1) * LANES)
        pre_in += iw_ref[:, span].astype(f32) * part
        pre_forget += fw_ref[:, span].astype(f32) * part
    input_pre = jnp.sum(pre_in, axis=1, keepdims=True)
    head_index = lax.broadcasted_iota(jnp.int32, (heads, 1), 0)
    bias = jnp.zeros((heads, 1), f32)
    old_max = jnp.zeros((heads, 1), f32)
    for h in range(heads):
        bias = jnp.where(head_index == h, fb_ref[h], bias)
        old_max = jnp.where(head_index == h, max_ref[0, h], old_max)
    forget_pre = jnp.sum(pre_forget, axis=1, keepdims=True) + bias
    log_forget = -(
        jnp.maximum(-forget_pre, 0.0) + jnp.log1p(jnp.exp(-jnp.abs(forget_pre)))
    )
    next_max = jnp.maximum(log_forget + old_max, input_pre)
    keep = jnp.exp(log_forget + old_max - next_max)
    admit = jnp.exp(input_pre - next_max)
    diag = lax.broadcasted_iota(jnp.int32, (heads, heads), 0) == lax.broadcasted_iota(
        jnp.int32, (heads, heads), 1
    )
    nmax_ref[...] = jnp.sum(jnp.where(diag, next_max, 0.0), axis=0, keepdims=True)

    r_index = lax.broadcasted_iota(jnp.int32, (pad4, head_dim), 0)
    j_index = lax.broadcasted_iota(jnp.int32, (pad4, head_dim), 1)
    if cols & (cols - 1) == 0:
        same = ((r_index ^ j_index) & (cols - 1)) == 0
    else:
        same = lax.rem(r_index, cols) == lax.rem(j_index, cols)
    spread[...] = jnp.where(same, 1.0, 0.0).astype(bf16)
    if pad4 != 4 * cols:
        w_in[pl.ds(4 * cols, pad4 - 4 * cols), :] = jnp.zeros((pad4 - 4 * cols, width), bf16)

    for copy in loads[6:10]:
        copy.wait()
    whole(0, rb1).wait_recv()
    rows = rb1[...].astype(f32)
    squares = jnp.sum(jnp.sum(rows * rows, axis=2, keepdims=True), axis=1, keepdims=True) / width
    normed = rows * lax.rsqrt(squares + norm_eps) * gain_ref[...][None]
    flat[...] = normed.reshape(n * blocks, LANES)
    for s in range(blocks):
        lhs[:, s * LANES : (s + 1) * LANES] = flat[pl.ds(s, n, stride=blocks), :].astype(bf16)
    result = lax.dot_general(lhs[...], w_in[...], NT, preferred_element_type=f32)
    result = result.astype(bf16).astype(f32)
    for t in range(n):
        sb2[t] = result[t : t + 1, :]
    rb2[pl.ds(me, 1)] = sb2[pl.ds(me, 1)]
    send_all(1, lambda peer: sb2.at[peer], rb2)

    loads[14].wait()
    for h in range(heads):
        block = mem[h]
        high = block.astype(bf16)
        mem_hi[h] = high
        mem_lo[h] = (block - high.astype(f32)).astype(bf16)

    for copy in loads[10:14]:
        copy.wait()
    whole(1, rb2).wait_recv()
    for d in range(n):
        x2[pl.ds(d, 1), :] = rb2[d]
    got = x2[...]
    lane = lax.broadcasted_iota(jnp.int32, (n, pad4), 1)
    stacked = jnp.concatenate(
        [
            jnp.where((lane >= m * cols) & (lane < (m + 1) * cols), got, 0.0).astype(bf16)
            for m in range(4)
        ],
        axis=0,
    )
    wide = jnp.dot(stacked, spread[...], preferred_element_type=f32)
    per_head = n // heads
    wide = wide.reshape(4 * heads, per_head, head_dim)
    d_index = lax.broadcasted_iota(jnp.int32, (1, per_head, head_dim), 1)
    lane = lax.broadcasted_iota(jnp.int32, (1, per_head, head_dim), 2)
    here = (lane >= d_index * cols) & (lane < (d_index + 1) * cols)
    vectors = jnp.sum(jnp.where(here, wide, 0.0), axis=1)
    query = vectors[:heads]
    key = vectors[heads : 2 * heads] * head_dim ** (-0.5)
    value = vectors[2 * heads : 3 * heads]
    outgate = vectors[3 * heads :]
    query_bf = query.astype(bf16)
    carried = []
    for h in range(heads):
        both = lax.dot_general(
            query_bf, mem_hi[h], NT, preferred_element_type=f32
        ) + lax.dot_general(query_bf, mem_lo[h], NT, preferred_element_type=f32)
        carried.append(both[h : h + 1, :])
    carried = jnp.concatenate(carried, axis=0)
    score = jnp.sum(key * query, axis=1, keepdims=True)
    old_norm = norm_ref[...]
    numer = keep * carried + (admit * score) * value
    denom = keep * jnp.sum(old_norm * query, axis=1, keepdims=True) + admit * score
    head_out = numer / jnp.maximum(jnp.abs(denom), jnp.exp(-next_max))
    gated = head_out * jax.nn.sigmoid(outgate)
    per = head_dim // LANES
    for b in range(per):
        row16[pl.ds(b, heads, stride=per), :] = gated[:, b * LANES : (b + 1) * LANES]
    sb3[...] = row16[...].astype(bf16)
    rb3[pl.ds(me, 1)] = sb3[...][None]
    send_all(2, lambda peer: sb3, rb3)
    nnorm_ref[...] = keep * old_norm + admit * key
    added = admit * value
    for h in range(heads):
        column = jnp.transpose(jnp.broadcast_to(added[h : h + 1, :], (LANES, head_dim)))
        kept = jnp.broadcast_to(keep[h : h + 1, :], (head_dim, LANES))
        for b in range(per):
            span = slice(b * LANES, (b + 1) * LANES)
            nmat_ref[h, :, span] = kept * mem[h, :, span] + column * key[h : h + 1, span]

    loads[15].wait()
    whole(2, rb3).wait_recv()
    flat[...] = rb3[...].astype(f32).reshape(n * blocks, LANES)
    for s in range(blocks):
        lhs[:, s * LANES : (s + 1) * LANES] = flat[pl.ds(s, n, stride=blocks), :].astype(bf16)
    proj = lax.dot_general(lhs[...], w_out[...], NT, preferred_element_type=f32)
    fold = LANES // cols
    piece = n // fold
    proj = proj.astype(bf16).astype(f32)
    sb4[...] = jnp.concatenate(
        [proj[f * piece : (f + 1) * piece, :] for f in range(fold)], axis=1
    ).astype(bf16)
    rb4[pl.ds(me, 1)] = sb4[...][None]
    send_all(3, lambda peer: sb4, rb4)
    flat[...] = rb1[...].astype(f32).reshape(n * blocks, LANES)

    whole(3, rb4).wait_recv()
    lane = lax.broadcasted_iota(jnp.int32, (piece, LANES), 1)
    squares = jnp.zeros((n, LANES), f32)
    for s in range(blocks):
        pieces = [rb4[s * fold + g].astype(f32) for g in range(fold)]
        parts = []
        for f in range(fold):
            made = pieces[0] if f == 0 else pltpu.roll(pieces[0], (-f * cols) % LANES, 1)
            for g in range(1, fold):
                moved = (
                    pieces[g] if g == f else pltpu.roll(pieces[g], ((g - f) * cols) % LANES, 1)
                )
                made = jnp.where(lane >= g * cols, moved, made)
            parts.append(made)
        projected = jnp.concatenate(parts, axis=0)
        mid = (flat[pl.ds(s, n, stride=blocks), :] + projected).astype(bf16).astype(f32)
        middle[:, s * LANES : (s + 1) * LANES] = mid
        squares += mid * mid
    inverse = lax.rsqrt(jnp.sum(squares, axis=1, keepdims=True) / width + norm_eps)
    for s in range(blocks):
        span = slice(s * LANES, (s + 1) * LANES)
        lhs[:, span] = (middle[:, span] * inverse * egain_ref[pl.ds(s, 1), :]).astype(bf16)
    for copy in loads[16:]:
        copy.wait()
    gate_part = jnp.dot(lhs[...], w_gate[...], preferred_element_type=f32)
    up_part = jnp.dot(lhs[...], w_up[...], preferred_element_type=f32)
    hidden = (gate_part / (1.0 + jnp.exp(-gate_part)) * up_part).astype(bf16)
    finished = jnp.dot(hidden, w_down[...], preferred_element_type=f32)
    for s in range(blocks):
        flat[pl.ds(s, n, stride=blocks), :] = finished[:, s * LANES : (s + 1) * LANES]
    sb5[...] = flat[...].astype(bf16).reshape(n, blocks, LANES)
    rb5[pl.ds(me, 1)] = sb5[pl.ds(me, 1)]
    send_all(4, lambda peer: sb5.at[peer], rb5)

    own_middle = middle[pl.ds(me, 1), :]
    for s in range(blocks):
        row16[pl.ds(s, 1), :] = own_middle[:, s * LANES : (s + 1) * LANES]
    whole(4, rb5).wait_recv()
    mixture = jnp.zeros((blocks, LANES), f32)
    for j in range(member_ref.shape[1]):
        chosen = group_ref[0] * members + member_ref[0, j]
        weight = gw_ref[0] * mw_ref[0, j]
        mixture += weight * rb5[chosen].astype(f32)
    row16[...] = row16[...] + mixture
    final = row16[...]
    for s in range(blocks):
        out_ref[:, s * LANES : (s + 1) * LANES] = final[s : s + 1, :].astype(bf16)
    whole(0, rb1).wait_send()
    whole(1, rb2).wait_send()
    whole(2, rb3).wait_send()
    whole(3, rb4).wait_send()
    whole(4, rb5).wait_send()


def store(heads, row, mat, nrm, top, row_out, mat_out, nrm_out, top_out, sem):
    pairs = [(mat.at[h], mat_out.at[h]) for h in range(heads)]
    pairs += [(row, row_out), (nrm, nrm_out), (top, top_out)]
    copies = [
        pltpu.make_async_copy(src, dst, sem.at[i]) for i, (src, dst) in enumerate(pairs)
    ]
    for copy in copies:
        copy.start()
    for copy in copies:
        copy.wait()


def pin(x):
    return pltpu.with_memory_space_constraint(x, pltpu.HBM)


def local(
    tokens,
    mixer_gain,
    query_weight,
    key_weight,
    value_weight,
    outgate_weight,
    input_weight,
    forget_weight,
    forget_bias,
    memory_matrix,
    memory_norm,
    memory_max,
    mixer_out,
    expert_gain,
    expert_gate,
    expert_up,
    expert_down,
    route_group,
    route_member,
    group_weight,
    member_weight,
):
    n = lax.axis_size("ep")
    assert tokens.shape[0] == 1 and expert_gate.shape[0] == 1
    width = tokens.shape[1]
    cols = query_weight.shape[1]
    heads, head_dim = memory_matrix.shape[1:3]
    hidden = expert_gate.shape[2]
    blocks = width // LANES
    members = n * expert_gate.shape[0] // GROUPS
    pad4 = -(-4 * cols // LANES) * LANES
    fold = LANES // cols
    f32, bf16, i32 = jnp.float32, jnp.bfloat16, jnp.int32
    vmem = pl.BlockSpec(memory_space=pltpu.VMEM)
    smem = pl.BlockSpec(memory_space=pltpu.SMEM)
    hbm = pl.BlockSpec(memory_space=pltpu.HBM)
    outs = pl.pallas_call(
        functools.partial(kernel, n, cols, members),
        out_shape=(
            jax.ShapeDtypeStruct((1, width), bf16),
            jax.ShapeDtypeStruct((heads, head_dim, head_dim), f32),
            jax.ShapeDtypeStruct((heads, head_dim), f32),
            jax.ShapeDtypeStruct((1, heads), f32),
        ),
        in_specs=[hbm] * 17 + [smem, hbm, smem, hbm],
        out_specs=(vmem,) * 4,
        scratch_shapes=[
            pltpu.VMEM((1, width), bf16),
            pltpu.VMEM((blocks, LANES), f32),
            pltpu.VMEM((blocks, LANES), f32),
            pltpu.VMEM((heads, width), bf16),
            pltpu.VMEM((heads, width), bf16),
            pltpu.SMEM((heads,), f32),
            pltpu.VMEM((heads, head_dim), f32),
            pltpu.SMEM((1, heads), f32),
            pltpu.SMEM((1, route_member.shape[1]), i32),
            pltpu.SMEM((1, route_member.shape[1]), f32),
            pltpu.VMEM((pad4, width), bf16),
            pltpu.VMEM((cols, width), bf16),
            pltpu.VMEM((heads, head_dim, head_dim), f32),
            pltpu.VMEM((heads, head_dim, head_dim), bf16),
            pltpu.VMEM((heads, head_dim, head_dim), bf16),
            pltpu.VMEM((width, hidden), bf16),
            pltpu.VMEM((width, hidden), bf16),
            pltpu.VMEM((hidden, width), bf16),
            pltpu.VMEM((pad4, head_dim), bf16),
            pltpu.VMEM((blocks, LANES), f32),
            pltpu.VMEM((blocks, LANES), bf16),
            pltpu.VMEM((n, blocks, LANES), bf16),
            pltpu.VMEM((n, 1, pad4), f32),
            pltpu.VMEM((n, 1, pad4), f32),
            pltpu.VMEM((n, pad4), f32),
            pltpu.VMEM((blocks, LANES), bf16),
            pltpu.VMEM((n, blocks, LANES), bf16),
            pltpu.VMEM((n // fold, LANES), bf16),
            pltpu.VMEM((n, n // fold, LANES), bf16),
            pltpu.VMEM((n, blocks, LANES), bf16),
            pltpu.VMEM((n, blocks, LANES), bf16),
            pltpu.VMEM((n * blocks, LANES), f32),
            pltpu.VMEM((n, width), bf16),
            pltpu.VMEM((n, width), f32),
            pltpu.SemaphoreType.DMA((19,)),
            pltpu.SemaphoreType.DMA((5,)),
            pltpu.SemaphoreType.DMA((5,)),
        ],
        compiler_params=pltpu.CompilerParams(
            collective_id=0, has_side_effects=True, vmem_limit_bytes=48 * 1024 * 1024
        ),
    )(
        pin(tokens),
        pin(mixer_gain.reshape(blocks, LANES)),
        pin(expert_gain.reshape(blocks, LANES)),
        pin(query_weight.T),
        pin(key_weight.T),
        pin(value_weight.T),
        pin(outgate_weight.T),
        pin(input_weight.T),
        pin(forget_weight.T),
        pin(forget_bias),
        pin(memory_matrix[0]),
        pin(memory_norm[0]),
        pin(memory_max),
        pin(mixer_out.T),
        pin(expert_gate[0]),
        pin(expert_up[0]),
        pin(expert_down[0]),
        route_group,
        pin(route_member),
        group_weight,
        pin(member_weight),
    )
    layer_out, next_matrix, next_norm, next_max = pl.pallas_call(
        functools.partial(store, heads),
        out_shape=tuple(jax.ShapeDtypeStruct(o.shape, o.dtype) for o in outs),
        in_specs=[vmem] * 4,
        out_specs=(hbm,) * 4,
        scratch_shapes=[pltpu.SemaphoreType.DMA((heads + 3,))],
        compiler_params=pltpu.CompilerParams(vmem_limit_bytes=1024 * 1024),
    )(*outs)
    return (layer_out, next_matrix[None], next_norm[None], next_max)


def solution(mesh):
    placed = (
        P("ep", None),
        P(),
        P(None, "ep"),
        P(None, "ep"),
        P(None, "ep"),
        P(None, "ep"),
        P(),
        P(),
        P(),
        P("ep", None, None, None),
        P("ep", None, None),
        P("ep", None),
        P(None, "ep"),
        P(),
        P("ep", None, None),
        P("ep", None, None),
        P("ep", None, None),
        P("ep"),
        P("ep", None),
        P("ep"),
        P("ep", None),
    )
    return jax.shard_map(
        local,
        mesh=mesh,
        in_specs=placed,
        out_specs=(P("ep", None), P("ep", None, None, None), P("ep", None, None), P("ep", None)),
        check_vma=False,
    )
```

```python
import functools

import jax
import jax.numpy as jnp
from jax import lax
from jax.experimental import pallas as pl
from jax.experimental.pallas import tpu as pltpu
from jax.sharding import PartitionSpec as P

GROUPS = 4
LANES = 128
norm_eps = 1e-06
MESH = pl.DeviceIdType.MESH
NT = (((1,), (1,)), ((), ()))


def kernel(
    n,
    cols,
    members,
    tokens_hbm,
    gain_hbm,
    egain_hbm,
    q_hbm,
    k_hbm,
    v_hbm,
    o_hbm,
    iw_hbm,
    fw_hbm,
    fb_hbm,
    mem_hbm,
    norm_hbm,
    max_hbm,
    mo_hbm,
    gate_hbm,
    up_hbm,
    down_hbm,
    group_ref,
    member_hbm,
    gw_ref,
    mw_hbm,
    out_ref,
    nmat_ref,
    nnorm_ref,
    nmax_ref,
    tokens_ref,
    gain_ref,
    egain_ref,
    iw_ref,
    fw_ref,
    fb_ref,
    norm_ref,
    max_ref,
    member_ref,
    mw_ref,
    w_in,
    w_out,
    mem,
    mem_hi,
    mem_lo,
    w_gate,
    w_up,
    w_down,
    spread,
    row16,
    sb1,
    rb1,
    sb2,
    rb2,
    x2,
    sb3,
    rb3,
    sb4,
    rb4,
    sb5,
    rb5,
    flat,
    lhs,
    middle,
    load_sem,
    send_sem,
    recv_sem,
):
    me = lax.axis_index("ep")
    width = tokens_ref.shape[1]
    blocks = width // LANES
    heads, head_dim = norm_ref.shape
    pad4 = w_in.shape[0]
    f32 = jnp.float32
    bf16 = jnp.bfloat16

    half = me // (n // 2)
    first = me + (1 - half) * n
    turn = 2 * half - 1

    def each_peer(body):
        chunk = 8
        full = (n - 1) // chunk

        def several(k, carry):
            for u in range(chunk):
                body(lax.rem(first + turn * (k * chunk + u + 1), n))
            return carry

        lax.fori_loop(0, full, several, 0)
        for u in range(full * chunk + 1, n):
            body(lax.rem(first + turn * u, n))

    barrier = pltpu.get_barrier_semaphore()

    def greet(peer):
        pl.semaphore_signal(barrier, inc=1, device_id=(peer,), device_id_type=MESH)

    each_peer(greet)

    loads = []
    for src, dst in (
        (tokens_hbm, tokens_ref),
        (gain_hbm, gain_ref),
        (iw_hbm, iw_ref),
        (fw_hbm, fw_ref),
        (fb_hbm, fb_ref),
        (max_hbm, max_ref),
        (q_hbm, w_in.at[pl.ds(0, cols)]),
        (k_hbm, w_in.at[pl.ds(cols, cols)]),
        (v_hbm, w_in.at[pl.ds(2 * cols, cols)]),
        (o_hbm, w_in.at[pl.ds(3 * cols, cols)]),
        (norm_hbm, norm_ref),
        (egain_hbm, egain_ref),
        (member_hbm, member_ref),
        (mw_hbm, mw_ref),
        (mem_hbm, mem),
        (mo_hbm, w_out),
        (gate_hbm, w_gate),
        (up_hbm, w_up),
        (down_hbm, w_down),
    ):
        copy = pltpu.make_async_copy(src, dst, load_sem.at[len(loads)])
        copy.start()
        loads.append(copy)

    def send_all(phase, source, target):
        def one(peer):
            pltpu.make_async_remote_copy(
                src_ref=source(peer),
                dst_ref=target.at[me],
                send_sem=send_sem.at[phase],
                recv_sem=recv_sem.at[phase],
                device_id=(peer,),
                device_id_type=MESH,
            ).start()

        each_peer(one)

    def whole(phase, target):
        view = target.at[pl.ds(0, n - 1)]
        return pltpu.make_async_remote_copy(
            src_ref=view,
            dst_ref=view,
            send_sem=send_sem.at[phase],
            recv_sem=recv_sem.at[phase],
            device_id=(lax.rem(me + 1, n),),
            device_id_type=MESH,
        )

    loads[0].wait()
    tok = tokens_ref[...].astype(f32)
    for s in range(blocks):
        row16[pl.ds(s, 1), :] = tok[:, s * LANES : (s + 1) * LANES]
    sb1[...] = row16[...].astype(bf16)
    rb1[pl.ds(me, 1)] = sb1[...][None]

    pl.semaphore_wait(barrier, n - 1)
    send_all(0, lambda peer: sb1, rb1)

    for copy in loads[1:6]:
        copy.wait()
    own = row16[...]
    scale = lax.rsqrt(
        jnp.sum(jnp.sum(own * own, axis=1, keepdims=True), axis=0, keepdims=True) / width + norm_eps
    )
    own_normed = (own * scale * gain_ref[...]).astype(bf16).astype(f32)
    pre_in = jnp.zeros((heads, LANES), f32)
    pre_forget = jnp.zeros((heads, LANES), f32)
    for s in range(blocks):
        part = own_normed[s : s + 1, :]
        span = slice(s * LANES, (s + 1) * LANES)
        pre_in += iw_ref[:, span].astype(f32) * part
        pre_forget += fw_ref[:, span].astype(f32) * part
    input_pre = jnp.sum(pre_in, axis=1, keepdims=True)
    head_index = lax.broadcasted_iota(jnp.int32, (heads, 1), 0)
    bias = jnp.zeros((heads, 1), f32)
    old_max = jnp.zeros((heads, 1), f32)
    for h in range(heads):
        bias = jnp.where(head_index == h, fb_ref[h], bias)
        old_max = jnp.where(head_index == h, max_ref[0, h], old_max)
    forget_pre = jnp.sum(pre_forget, axis=1, keepdims=True) + bias
    log_forget = -(
        jnp.maximum(-forget_pre, 0.0) + jnp.log1p(jnp.exp(-jnp.abs(forget_pre)))
    )
    next_max = jnp.maximum(log_forget + old_max, input_pre)
    keep = jnp.exp(log_forget + old_max - next_max)
    admit = jnp.exp(input_pre - next_max)
    diag = lax.broadcasted_iota(jnp.int32, (heads, heads), 0) == lax.broadcasted_iota(
        jnp.int32, (heads, heads), 1
    )
    nmax_ref[...] = jnp.sum(jnp.where(diag, next_max, 0.0), axis=0, keepdims=True)

    r_index = lax.broadcasted_iota(jnp.int32, (pad4, head_dim), 0)
    j_index = lax.broadcasted_iota(jnp.int32, (pad4, head_dim), 1)
    if cols & (cols - 1) == 0:
        same = ((r_index ^ j_index) & (cols - 1)) == 0
    else:
        same = lax.rem(r_index, cols) == lax.rem(j_index, cols)
    spread[...] = jnp.where(same, 1.0, 0.0).astype(bf16)
    if pad4 != 4 * cols:
        w_in[pl.ds(4 * cols, pad4 - 4 * cols), :] = jnp.zeros((pad4 - 4 * cols, width), bf16)

    for copy in loads[6:10]:
        copy.wait()
    whole(0, rb1).wait_recv()
    rows = rb1[...].astype(f32)
    squares = jnp.sum(jnp.sum(rows * rows, axis=2, keepdims=True), axis=1, keepdims=True) / width
    normed = rows * lax.rsqrt(squares + norm_eps) * gain_ref[...][None]
    flat[...] = normed.reshape(n * blocks, LANES)
    for s in range(blocks):
        lhs[:, s * LANES : (s + 1) * LANES] = flat[pl.ds(s, n, stride=blocks), :].astype(bf16)
    result = lax.dot_general(lhs[...], w_in[...], NT, preferred_element_type=f32)
    result = result.astype(bf16).astype(f32)
    for t in range(n):
        sb2[t] = result[t : t + 1, :]
    send_all(1, lambda peer: sb2.at[peer], rb2)
    rb2[pl.ds(me, 1)] = sb2[pl.ds(me, 1)]

    loads[14].wait()
    for h in range(heads):
        block = mem[h]
        high = block.astype(bf16)
        mem_hi[h] = high
        mem_lo[h] = (block - high.astype(f32)).astype(bf16)

    for copy in loads[10:14]:
        copy.wait()
    whole(1, rb2).wait_recv()
    for d in range(n):
        x2[pl.ds(d, 1), :] = rb2[d]
    got = x2[...]
    lane = lax.broadcasted_iota(jnp.int32, (n, pad4), 1)
    stacked = jnp.concatenate(
        [
            jnp.where((lane >= m * cols) & (lane < (m + 1) * cols), got, 0.0).astype(bf16)
            for m in range(4)
        ],
        axis=0,
    )
    wide = jnp.dot(stacked, spread[...], preferred_element_type=f32)
    per_head = n // heads
    wide = wide.reshape(4 * heads, per_head, head_dim)
    d_index = lax.broadcasted_iota(jnp.int32, (1, per_head, head_dim), 1)
    lane = lax.broadcasted_iota(jnp.int32, (1, per_head, head_dim), 2)
    here = (lane >= d_index * cols) & (lane < (d_index + 1) * cols)
    vectors = jnp.sum(jnp.where(here, wide, 0.0), axis=1)
    query = vectors[:heads]
    key = vectors[heads : 2 * heads] * head_dim ** (-0.5)
    value = vectors[2 * heads : 3 * heads]
    outgate = vectors[3 * heads :]
    query_bf = query.astype(bf16)
    carried = []
    for h in range(heads):
        both = lax.dot_general(
            query_bf, mem_hi[h], NT, preferred_element_type=f32
        ) + lax.dot_general(query_bf, mem_lo[h], NT, preferred_element_type=f32)
        carried.append(both[h : h + 1, :])
    carried = jnp.concatenate(carried, axis=0)
    score = jnp.sum(key * query, axis=1, keepdims=True)
    old_norm = norm_ref[...]
    numer = keep * carried + (admit * score) * value
    denom = keep * jnp.sum(old_norm * query, axis=1, keepdims=True) + admit * score
    head_out = numer / jnp.maximum(jnp.abs(denom), jnp.exp(-next_max))
    gated = head_out * jax.nn.sigmoid(outgate)
    per = head_dim // LANES
    for b in range(per):
        row16[pl.ds(b, heads, stride=per), :] = gated[:, b * LANES : (b + 1) * LANES]
    sb3[...] = row16[...].astype(bf16)
    send_all(2, lambda peer: sb3, rb3)
    rb3[pl.ds(me, 1)] = sb3[...][None]
    nnorm_ref[...] = keep * old_norm + admit * key
    added = admit * value
    for h in range(heads):
        column = jnp.transpose(jnp.broadcast_to(added[h : h + 1, :], (LANES, head_dim)))
        kept = jnp.broadcast_to(keep[h : h + 1, :], (head_dim, LANES))
        for b in range(per):
            span = slice(b * LANES, (b + 1) * LANES)
            nmat_ref[h, :, span] = kept * mem[h, :, span] + column * key[h : h + 1, span]

    loads[15].wait()
    whole(2, rb3).wait_recv()
    flat[...] = rb3[...].astype(f32).reshape(n * blocks, LANES)
    for s in range(blocks):
        lhs[:, s * LANES : (s + 1) * LANES] = flat[pl.ds(s, n, stride=blocks), :].astype(bf16)
    proj = lax.dot_general(lhs[...], w_out[...], NT, preferred_element_type=f32)
    fold = LANES // cols
    piece = n // fold
    proj = proj.astype(bf16).astype(f32)
    sb4[...] = jnp.concatenate(
        [proj[f * piece : (f + 1) * piece, :] for f in range(fold)], axis=1
    ).astype(bf16)
    send_all(3, lambda peer: sb4, rb4)
    rb4[pl.ds(me, 1)] = sb4[...][None]
    flat[...] = rb1[...].astype(f32).reshape(n * blocks, LANES)

    whole(3, rb4).wait_recv()
    lane = lax.broadcasted_iota(jnp.int32, (piece, LANES), 1)
    squares = jnp.zeros((n, LANES), f32)
    for s in range(blocks):
        pieces = [rb4[s * fold + g].astype(f32) for g in range(fold)]
        parts = []
        for f in range(fold):
            made = pieces[0] if f == 0 else pltpu.roll(pieces[0], (-f * cols) % LANES, 1)
            for g in range(1, fold):
                moved = (
                    pieces[g] if g == f else pltpu.roll(pieces[g], ((g - f) * cols) % LANES, 1)
                )
                made = jnp.where(lane >= g * cols, moved, made)
            parts.append(made)
        projected = jnp.concatenate(parts, axis=0)
        mid = (flat[pl.ds(s, n, stride=blocks), :] + projected).astype(bf16).astype(f32)
        middle[:, s * LANES : (s + 1) * LANES] = mid
        squares += mid * mid
    inverse = lax.rsqrt(jnp.sum(squares, axis=1, keepdims=True) / width + norm_eps)
    for s in range(blocks):
        span = slice(s * LANES, (s + 1) * LANES)
        lhs[:, span] = (middle[:, span] * inverse * egain_ref[pl.ds(s, 1), :]).astype(bf16)
    for copy in loads[16:]:
        copy.wait()
    gate_part = jnp.dot(lhs[...], w_gate[...], preferred_element_type=f32)
    up_part = jnp.dot(lhs[...], w_up[...], preferred_element_type=f32)
    hidden = (gate_part / (1.0 + jnp.exp(-gate_part)) * up_part).astype(bf16)
    finished = jnp.dot(hidden, w_down[...], preferred_element_type=f32)
    for s in range(blocks):
        flat[pl.ds(s, n, stride=blocks), :] = finished[:, s * LANES : (s + 1) * LANES]
    sb5[...] = flat[...].astype(bf16).reshape(n, blocks, LANES)
    send_all(4, lambda peer: sb5.at[peer], rb5)
    rb5[pl.ds(me, 1)] = sb5[pl.ds(me, 1)]

    own_middle = middle[pl.ds(me, 1), :]
    for s in range(blocks):
        row16[pl.ds(s, 1), :] = own_middle[:, s * LANES : (s + 1) * LANES]
    whole(4, rb5).wait_recv()
    mixture = jnp.zeros((blocks, LANES), f32)
    for j in range(member_ref.shape[1]):
        chosen = group_ref[0] * members + member_ref[0, j]
        weight = gw_ref[0] * mw_ref[0, j]
        mixture += weight * rb5[chosen].astype(f32)
    row16[...] = row16[...] + mixture
    final = row16[...]
    for s in range(blocks):
        out_ref[:, s * LANES : (s + 1) * LANES] = final[s : s + 1, :].astype(bf16)
    whole(0, rb1).wait_send()
    whole(1, rb2).wait_send()
    whole(2, rb3).wait_send()
    whole(3, rb4).wait_send()
    whole(4, rb5).wait_send()


def store(heads, row, mat, nrm, top, row_out, mat_out, nrm_out, top_out, sem):
    pairs = [(mat.at[h], mat_out.at[h]) for h in range(heads)]
    pairs += [(row, row_out), (nrm, nrm_out), (top, top_out)]
    copies = [
        pltpu.make_async_copy(src, dst, sem.at[i]) for i, (src, dst) in enumerate(pairs)
    ]
    for copy in copies:
        copy.start()
    for copy in copies:
        copy.wait()


def pin(x):
    return pltpu.with_memory_space_constraint(x, pltpu.HBM)


def local(
    tokens,
    mixer_gain,
    query_weight,
    key_weight,
    value_weight,
    outgate_weight,
    input_weight,
    forget_weight,
    forget_bias,
    memory_matrix,
    memory_norm,
    memory_max,
    mixer_out,
    expert_gain,
    expert_gate,
    expert_up,
    expert_down,
    route_group,
    route_member,
    group_weight,
    member_weight,
):
    n = lax.axis_size("ep")
    assert tokens.shape[0] == 1 and expert_gate.shape[0] == 1
    width = tokens.shape[1]
    cols = query_weight.shape[1]
    heads, head_dim = memory_matrix.shape[1:3]
    hidden = expert_gate.shape[2]
    blocks = width // LANES
    members = n * expert_gate.shape[0] // GROUPS
    pad4 = -(-4 * cols // LANES) * LANES
    fold = LANES // cols
    f32, bf16, i32 = jnp.float32, jnp.bfloat16, jnp.int32
    vmem = pl.BlockSpec(memory_space=pltpu.VMEM)
    smem = pl.BlockSpec(memory_space=pltpu.SMEM)
    hbm = pl.BlockSpec(memory_space=pltpu.HBM)
    outs = pl.pallas_call(
        functools.partial(kernel, n, cols, members),
        out_shape=(
            jax.ShapeDtypeStruct((1, width), bf16),
            jax.ShapeDtypeStruct((heads, head_dim, head_dim), f32),
            jax.ShapeDtypeStruct((heads, head_dim), f32),
            jax.ShapeDtypeStruct((1, heads), f32),
        ),
        in_specs=[hbm] * 17 + [smem, hbm, smem, hbm],
        out_specs=(vmem,) * 4,
        scratch_shapes=[
            pltpu.VMEM((1, width), bf16),
            pltpu.VMEM((blocks, LANES), f32),
            pltpu.VMEM((blocks, LANES), f32),
            pltpu.VMEM((heads, width), bf16),
            pltpu.VMEM((heads, width), bf16),
            pltpu.SMEM((heads,), f32),
            pltpu.VMEM((heads, head_dim), f32),
            pltpu.SMEM((1, heads), f32),
            pltpu.SMEM((1, route_member.shape[1]), i32),
            pltpu.SMEM((1, route_member.shape[1]), f32),
            pltpu.VMEM((pad4, width), bf16),
            pltpu.VMEM((cols, width), bf16),
            pltpu.VMEM((heads, head_dim, head_dim), f32),
            pltpu.VMEM((heads, head_dim, head_dim), bf16),
            pltpu.VMEM((heads, head_dim, head_dim), bf16),
            pltpu.VMEM((width, hidden), bf16),
            pltpu.VMEM((width, hidden), bf16),
            pltpu.VMEM((hidden, width), bf16),
            pltpu.VMEM((pad4, head_dim), bf16),
            pltpu.VMEM((blocks, LANES), f32),
            pltpu.VMEM((blocks, LANES), bf16),
            pltpu.VMEM((n, blocks, LANES), bf16),
            pltpu.VMEM((n, 1, pad4), f32),
            pltpu.VMEM((n, 1, pad4), f32),
            pltpu.VMEM((n, pad4), f32),
            pltpu.VMEM((blocks, LANES), bf16),
            pltpu.VMEM((n, blocks, LANES), bf16),
            pltpu.VMEM((n // fold, LANES), bf16),
            pltpu.VMEM((n, n // fold, LANES), bf16),
            pltpu.VMEM((n, blocks, LANES), bf16),
            pltpu.VMEM((n, blocks, LANES), bf16),
            pltpu.VMEM((n * blocks, LANES), f32),
            pltpu.VMEM((n, width), bf16),
            pltpu.VMEM((n, width), f32),
            pltpu.SemaphoreType.DMA((19,)),
            pltpu.SemaphoreType.DMA((5,)),
            pltpu.SemaphoreType.DMA((5,)),
        ],
        compiler_params=pltpu.CompilerParams(
            collective_id=0, has_side_effects=True, vmem_limit_bytes=48 * 1024 * 1024
        ),
    )(
        pin(tokens),
        pin(mixer_gain.reshape(blocks, LANES)),
        pin(expert_gain.reshape(blocks, LANES)),
        pin(query_weight.T),
        pin(key_weight.T),
        pin(value_weight.T),
        pin(outgate_weight.T),
        pin(input_weight.T),
        pin(forget_weight.T),
        pin(forget_bias),
        pin(memory_matrix[0]),
        pin(memory_norm[0]),
        pin(memory_max),
        pin(mixer_out.T),
        pin(expert_gate[0]),
        pin(expert_up[0]),
        pin(expert_down[0]),
        route_group,
        pin(route_member),
        group_weight,
        pin(member_weight),
    )
    layer_out, next_matrix, next_norm, next_max = pl.pallas_call(
        functools.partial(store, heads),
        out_shape=tuple(jax.ShapeDtypeStruct(o.shape, o.dtype) for o in outs),
        in_specs=[vmem] * 4,
        out_specs=(hbm,) * 4,
        scratch_shapes=[pltpu.SemaphoreType.DMA((heads + 3,))],
        compiler_params=pltpu.CompilerParams(vmem_limit_bytes=1024 * 1024),
    )(*outs)
    return (layer_out, next_matrix[None], next_norm[None], next_max)


def solution(mesh):
    placed = (
        P("ep", None),
        P(),
        P(None, "ep"),
        P(None, "ep"),
        P(None, "ep"),
        P(None, "ep"),
        P(),
        P(),
        P(),
        P("ep", None, None, None),
        P("ep", None, None),
        P("ep", None),
        P(None, "ep"),
        P(),
        P("ep", None, None),
        P("ep", None, None),
        P("ep", None, None),
        P("ep"),
        P("ep", None),
        P("ep"),
        P("ep", None),
    )
    return jax.shard_map(
        local,
        mesh=mesh,
        in_specs=placed,
        out_specs=(P("ep", None), P("ep", None, None, None), P("ep", None, None), P("ep", None)),
        check_vma=False,
    )
```
